32 devices in a mesh: fs: 8 (over z, x), tp: 4 (over y, core).
Axes of the slice: x: 2, y: 2, z: 4, core: 2. Of those that a mesh axis runs over, the one named last changes fastest.
Arguments:
- query_rows: bfloat16 [16384, 2048], P('fs', 'tp'), may hold values from -16 to 16
- key_rows: bfloat16 [16384, 2048], P('fs', 'tp'), may hold values from -8 to 8
- value_rows: bfloat16 [16384, 2048], P('fs', 'tp'), may hold values from -6 to 6
- mix_lambda: float32 [16], P('tp'), may hold values from 0.3 to 0.8
- head_gain: float32 [128], replicated, may hold values from 0.1 to 1.9
- out_cotangent: bfloat16 [16384, 2048], P('fs'), may hold values from -0.049804688 to 0.049804688
- layer_input: bfloat16 [16384, 2048], P('fs'), may hold values from -6 to 6
- value_cotangent: bfloat16 [16384, 2048], P('fs', 'tp'), may hold values from -0.049804688 to 0.049804688
- out_weight: float32 [2048, 2048], P('tp', 'fs'), may hold values from -0.125 to 0.125
- value_weight: float32 [2048, 2048], P('fs', 'tp'), may hold values from -0.125 to 0.125
- out_basis: bfloat16 [2048, 256], replicated, may hold values from -0.125 to 0.125
- value_basis: bfloat16 [2048, 256], replicated, may hold values from -0.125 to 0.125
- out_first: float32 [256, 2048], P('fs', 'tp'), may hold values from -20 to 20
- out_second: float32 [256, 2048], P('fs', 'tp'), may hold values from 0.02 to 0.5
- value_first: float32 [256, 2048], P('fs', 'tp'), may hold values from -20 to 20
- value_second: float32 [256, 2048], P('fs', 'tp'), may hold values from 0.02 to 0.5
Outputs:
- out_step: float32 [2048, 2048], P('tp', 'fs')
- value_step: float32 [2048, 2048], P('fs', 'tp')
- new_out_weight: float32 [2048, 2048], P('tp', 'fs')
- new_value_weight: float32 [2048, 2048], P('fs', 'tp')
- out_copy: bfloat16 [2048, 2048], P('tp')
- value_copy: bfloat16 [2048, 2048], P(None, 'tp')
- new_out_first: float32 [256, 2048], P('fs', 'tp')
- new_out_second: float32 [256, 2048], P('fs', 'tp')
- new_value_first: float32 [256, 2048], P('fs', 'tp')
- new_value_second: float32 [256, 2048], P('fs', 'tp')
The draws below stay inside these ranges and needn't reach their ends.
All inputs are finite; a program needn't handle non-finite values.
Results may differ from the reference program's by a relative error of at most 0.001.
Values may be sent and summed in bfloat16 or wider, within the bound.
A program may use at most 192 MiB of HBM per device.

```python
import math
import jax
import jax.numpy as jnp
from jax import lax

D = 2048
H = 16
DH = 64
DV = 128
RANK = 256
LEN = 2048
TOKENS = 16384
V = 2048
QKW = 2048


def draw_query_rows(key, part):
    base_draw = jnp.clip(jax.random.normal(jax.random.fold_in(key, 1), (TOKENS // LEN, LEN, 2 * H, DH), jnp.float32) * 1.3, -5.2, 5.2)
    return jnp.clip(base_draw, -16.0, 16.0).reshape(TOKENS, QKW).astype(jnp.bfloat16)


def draw_key_rows(key, part):
    base_draw = jnp.clip(jax.random.normal(jax.random.fold_in(key, 2), (TOKENS // LEN, LEN, 2 * H, DH), jnp.float32) * 1.3, -5.2, 5.2)
    return jnp.clip(base_draw, -8.0, 8.0).reshape(TOKENS, QKW).astype(jnp.bfloat16)


def moment_draw(key, salt):
    row_rise = jnp.arange(RANK, dtype=jnp.float32)[:, None] / RANK
    col_rise = jnp.arange(V, dtype=jnp.float32)[None, :] / V
    jitter = jax.random.uniform(jax.random.fold_in(key, salt), (RANK, V), jnp.float32, -0.35, 0.35)
    scales = 0.3 * 10.0 ** (0.5 * (row_rise + col_rise)) * jnp.exp(jitter)
    values = jnp.clip(jax.random.normal(jax.random.fold_in(key, salt + 1), (RANK, V), jnp.float32), -4.0, 4.0)
    return jnp.clip(values * scales, -20.0, 20.0)


def draw_out_first(key, part):
    return moment_draw(key, 11)


def draw_value_first(key, part):
    return moment_draw(key, 21)


def shard_levels(key, shape, split, least, top_value):
    level = 1.0
    for axis_at, parts in split:
        heights = jax.random.uniform(jax.random.fold_in(jax.random.fold_in(key, 6), axis_at), (parts,), jnp.float32, least / len(split), top_value / len(split))
        level = level * jnp.repeat(jnp.exp(heights), shape[axis_at] // parts).reshape((-1,) + (1,) * (len(shape) - 1 - axis_at))
    return level


def scatter_about(key, shape, spread, reach, pieces=(), kind=jnp.bfloat16):
    drawn = jax.random.normal(key, shape, jnp.float32) * spread
    if len(pieces) > 0:
        drawn = shard_levels(key, shape, pieces, -0.22, 0.18) * drawn
    return jnp.clip(drawn, min=-reach, max=reach).astype(kind)


def setup_inputs(seed: int = 0) -> dict:
    key_list = jax.random.split(jax.random.key(seed), 17)
    return {
        "query_rows": draw_query_rows(jax.random.fold_in(key_list[16], 71), 0),
        "key_rows": draw_key_rows(jax.random.fold_in(key_list[16], 71), 0),
        "value_rows": scatter_about(key_list[2], (TOKENS, V), 1.0, 6.0, ((0, 8), (1, 4))),
        "mix_lambda": jnp.clip(0.3 + 0.5 * jax.random.uniform(key_list[3], (H,), jnp.float32) ** shard_levels(key_list[3], (H,), ((0, 4),), -0.2, 0.2), 0.3, 0.8),
        "head_gain": jnp.clip(1.0 + 0.18 * jax.random.normal(key_list[4], (DV,), jnp.float32), 0.1, 1.9),
        "out_cotangent": scatter_about(key_list[5], (TOKENS, D), 0.008, 0.049804688, ((0, 8),)),
        "layer_input": scatter_about(key_list[6], (TOKENS, D), 1.0, 6.0, ((0, 8),)),
        "value_cotangent": scatter_about(key_list[7], (TOKENS, V), 0.008, 0.049804688, ((0, 8), (1, 4))),
        "out_weight": scatter_about(key_list[8], (V, D), V ** -0.5, 0.125, ((0, 4), (1, 8)), jnp.float32),
        "value_weight": scatter_about(key_list[9], (D, V), D ** -0.5, 0.125, ((0, 8), (1, 4)), jnp.float32),
        "out_basis": scatter_about(key_list[10], (D, RANK), D ** -0.5, 0.125),
        "value_basis": scatter_about(key_list[11], (D, RANK), D ** -0.5, 0.125),
        "out_first": draw_out_first(jax.random.fold_in(key_list[16], 71), 0),
        "out_second": jnp.clip(jnp.exp(math.log(0.5) - 3.218876 * jax.random.uniform(key_list[13], (RANK, V), jnp.float32) ** shard_levels(key_list[13], (RANK, V), ((0, 8), (1, 4)), -0.2, 0.2)), 0.02, 0.5),
        "value_first": draw_value_first(jax.random.fold_in(key_list[16], 71), 0),
        "value_second": jnp.clip(jnp.exp(math.log(0.5) - 3.218876 * jax.random.uniform(key_list[15], (RANK, V), jnp.float32) ** shard_levels(key_list[15], (RANK, V), ((0, 8), (1, 4)), -0.2, 0.2)), 0.02, 0.5),
    }


EPSILON_NORM = 1e-05
EPSILON_ADAM = 1e-08
BETA_ONE = 0.9
BETA_TWO = 0.95
CLIP_RMS = 1.0
LEARN_RATE = 0.01

def moment_step(proj, first, second):
    new_first = BETA_ONE * first + (1.0 - BETA_ONE) * proj
    new_second = BETA_TWO * second + (1.0 - BETA_TWO) * proj * proj
    direction = new_first / (jnp.sqrt(new_second) + EPSILON_ADAM)
    return (new_first, new_second, direction)

def adapt(grad, basis, first, second):
    basis_wide = basis.astype(jnp.float32)
    proj = jnp.dot(basis_wide.T, grad, precision=lax.Precision.HIGHEST)
    new_first, new_second, direction = moment_step(proj, first, second)
    clip_factor = jnp.minimum(1.0, CLIP_RMS * math.sqrt(RANK * V) / jnp.sqrt(jnp.sum(direction * direction)))
    step_full = clip_factor * jnp.dot(basis_wide, direction, precision=lax.Precision.HIGHEST)
    return (step_full, new_first, new_second)

def reference(query_rows, key_rows, value_rows, mix_lambda, head_gain, out_cotangent, layer_input, value_cotangent, out_weight, value_weight, out_basis, value_basis, out_first, out_second, value_first, value_second):
    seq_count = TOKENS // LEN
    query_heads = query_rows.reshape(seq_count, LEN, H, 2, DH).transpose(0, 2, 3, 1, 4).reshape(seq_count * H, 2, LEN, DH)
    key_heads = key_rows.reshape(seq_count, LEN, H, 2, DH).transpose(0, 2, 3, 1, 4).reshape(seq_count * H, 2, LEN, DH)
    value_heads = value_rows.reshape(seq_count, LEN, H, DV).transpose(0, 2, 1, 3).reshape(seq_count * H, LEN, DV)
    lam_rows = jnp.tile(mix_lambda, seq_count)
    positions = jnp.arange(LEN)
    causal = positions[None, :] <= positions[:, None]

    def attend(operands):
        query_pair, key_pair, value_head, lam_value = operands
        scores = jnp.einsum('mqd,mkd->mqk', query_pair.astype(jnp.float32), key_pair.astype(jnp.float32)) * DH ** (-0.5)
        scores = jnp.where(causal[None], scores, -jnp.inf)
        row_peak = lax.optimization_barrier(jnp.max(scores, axis=-1, keepdims=True))
        exp_scores = jnp.exp(scores - row_peak)
        soft_maps = exp_scores / lax.optimization_barrier(jnp.sum(exp_scores, axis=-1, keepdims=True))
        mix_weights = (soft_maps[0] - lam_value * soft_maps[1]).astype(jnp.bfloat16)
        raw_out = jnp.dot(mix_weights, value_head, preferred_element_type=jnp.float32)
        normed = raw_out * lax.rsqrt(lax.optimization_barrier(jnp.mean(raw_out * raw_out, axis=-1, keepdims=True)) + EPSILON_NORM) * head_gain
        return normed.astype(jnp.bfloat16)
    head_blocks = lax.map(attend, (query_heads, key_heads, value_heads, lam_rows))
    head_out = head_blocks.reshape(seq_count, H, LEN, DV).transpose(0, 2, 1, 3).reshape(TOKENS, H * DV)
    out_grad = jnp.dot(out_cotangent.T, head_out, preferred_element_type=jnp.float32)
    value_grad = jnp.dot(layer_input.T, value_cotangent, preferred_element_type=jnp.float32)
    out_full, new_out_first, new_out_second = adapt(out_grad, out_basis, out_first, out_second)
    value_step, new_value_first, new_value_second = adapt(value_grad, value_basis, value_first, value_second)
    out_step = out_full.T
    new_out_weight = out_weight - LEARN_RATE * out_step
    new_value_weight = value_weight - LEARN_RATE * value_step
    return (out_step, value_step, new_out_weight, new_value_weight, new_out_weight.astype(jnp.bfloat16), new_value_weight.astype(jnp.bfloat16), new_out_first, new_out_second, new_value_first, new_value_second)
```

```python
import functools
import math

import jax
import jax.numpy as jnp
from jax import lax
from jax.experimental import pallas as pl
from jax.experimental.pallas import tpu as pltpu
from jax.sharding import PartitionSpec as P

DH = 64
DV = 128


EPSILON_NORM = 1e-05
EPSILON_ADAM = 1e-08
BETA_ONE = 0.9
BETA_TWO = 0.95
CLIP_RMS = 1.0
LEARN_RATE = 0.01
TILE = 256
SLOTS = 4
PAIR = 2
LOG2E = 1.4426950408889634
F32 = jnp.float32
BF16 = jnp.bfloat16


def dot_f32(left, right, dims=((1,), (0,))):
    return lax.dot_general(left, right, (dims, ((), ())), preferred_element_type=F32)


def split_two(wide):
    high = wide.astype(BF16)
    return high, (wide - high.astype(F32)).astype(BF16)


def fold_rows(tile, op):
    rows, cols = tile.shape
    return op(tile.reshape(rows // 8, 8, cols), axis=0)


def moment_step(proj, first, second):
    new_first = BETA_ONE * first + (1.0 - BETA_ONE) * proj
    new_second = BETA_TWO * second + (1.0 - BETA_TWO) * proj * proj
    direction = new_first / (jnp.sqrt(new_second) + EPSILON_ADAM)
    return (new_first, new_second, direction)


def step_kernel(
    fs_count, tp_count,
    lam_ref, gain_ref, query_h, key_h, value_h, cot_h, input_h, vcot_h, obasis_h, vbasis_h,
    oweight_h, vweight_h, ofirst_h, osecond_h, vfirst_h, vsecond_h,
    ostep, vstep, onew, vnew, ocopy, vcopy, ofirst_new, osecond_new, vfirst_new, vsecond_new,
    query_v, key_v, value_v, vcot_v, obasis_v, vbasis_v, oweight, vweight,
    ofirst, osecond, vfirst, vsecond, chunks,
    score_one, score_two, mix_ref, value_t, obasis_t, vbasis_t, cb_high, cb_low, gain_t, tri,
    vproj, oproj, vgot, ogot, vdirs, odirs, squares, squares_got,
    load_sem, chunk_sem, vs_send, vs_recv, os_send, os_recv, vg_send, vg_recv, og_send, og_recv,
    sq_send, sq_recv, ring_send, ring_recv,
):
    me = lax.axis_index("fs")
    my_tp = lax.axis_index("tp")
    half_count = fs_count // 2
    rank_share, cols = ofirst.shape
    row_share = vweight.shape[0]
    seq_len = query_v.shape[0]
    blocks = seq_len // TILE
    pairs = oproj.shape[0]
    wide = PAIR * DV
    mesh_ids = pl.DeviceIdType.MESH

    def fs_peer(gap):
        return lax.rem(me + gap, fs_count)

    def tp_peer(gap):
        return lax.rem(my_tp + gap, tp_count)

    def share(index, size):
        return pl.ds(pl.multiple_of(index * size, size), size)

    barrier = pltpu.get_barrier_semaphore()
    for gap in range(1, fs_count):
        pl.semaphore_signal(
            barrier, inc=1, device_id=(fs_peer(gap), my_tp), device_id_type=mesh_ids
        )
    for gap in range(1, tp_count):
        pl.semaphore_signal(
            barrier, inc=1, device_id=(me, tp_peer(gap)), device_id_type=mesh_ids
        )

    def chunk_copy(source, at, slot):
        return pltpu.make_async_copy(
            source.at[share(at, TILE)], chunks.at[slot], chunk_sem.at[slot]
        )

    def load(index, source, target):
        copy = pltpu.make_async_copy(source, target, load_sem.at[index])
        copy.start()
        return copy

    early = [load(0, vbasis_h, vbasis_v)]
    for at in range(SLOTS - 1):
        chunk_copy(input_h, at, at).start()
    early.append(load(1, vcot_h, vcot_v))
    chunk_copy(input_h, SLOTS - 1, SLOTS - 1).start()
    early.append(load(2, obasis_h, obasis_v))
    attention = [
        load(3, query_h, query_v), load(4, key_h, key_v), load(5, value_h, value_v),
    ]
    late = [
        load(6, vfirst_h, vfirst), load(7, vsecond_h, vsecond), load(8, ofirst_h, ofirst),
        load(9, osecond_h, osecond), load(10, vweight_h, vweight), load(11, oweight_h, oweight),
    ]

    key_pos = lax.broadcasted_iota(jnp.int32, (TILE, TILE), 0)
    query_pos = lax.broadcasted_iota(jnp.int32, (TILE, TILE), 1)
    tri[...] = jnp.where(key_pos <= query_pos, 0.0, -jnp.inf)
    gain_t[...] = jnp.broadcast_to(gain_ref[...], (DV, DV)).T
    vproj[...] = jnp.zeros_like(vproj)
    oproj[...] = jnp.zeros_like(oproj)

    early[0].wait()
    vbasis_t[...] = vbasis_v[...].T
    early[1].wait()

    def value_block(at, carry):
        slot = lax.rem(at, SLOTS)
        chunk_copy(input_h, at, slot).wait()
        high, low = split_two(dot_f32(vbasis_t[...], chunks[slot], ((1,), (1,))))
        vcot = vcot_v[share(at, TILE), :]
        vproj[...] += dot_f32(high, vcot) + dot_f32(low, vcot)

        @pl.when(at < blocks - SLOTS)
        def _():
            chunk_copy(input_h, at + SLOTS, slot).start()

        @pl.when(at >= blocks - SLOTS)
        def _():
            chunk_copy(cot_h, at - (blocks - SLOTS), slot).start()

        return carry

    lax.fori_loop(0, blocks, value_block, 0)
    pl.semaphore_wait(barrier, fs_count + tp_count - 2)

    def exchange(source, target, send, recv):
        copies = []
        for gap in range(1, fs_count):
            peer = fs_peer(gap)
            copies.append(
                pltpu.make_async_remote_copy(
                    src_ref=source(peer),
                    dst_ref=target(gap),
                    send_sem=send.at[gap - 1],
                    recv_sem=recv.at[gap - 1],
                    device_id=(peer, my_tp),
                    device_id_type=mesh_ids,
                )
            )
        return copies

    vscatter = exchange(
        lambda peer: vproj.at[share(peer, rank_share)], lambda gap: vgot.at[gap - 1],
        vs_send, vs_recv,
    )
    vgather = exchange(
        lambda peer: vdirs.at[share(me, rank_share)],
        lambda gap: vdirs.at[share(me, rank_share)], vg_send, vg_recv,
    )
    oscatter = [
        exchange(
            lambda peer, at=at: oproj.at[at, share(peer, rank_share)],
            lambda gap, at=at: ogot.at[at, gap - 1], os_send.at[at], os_recv.at[at],
        )
        for at in range(pairs)
    ]
    ogather = [
        exchange(
            lambda peer, at=at: odirs.at[at, share(me, rank_share)],
            lambda gap, at=at: odirs.at[at, share(me, rank_share)],
            og_send.at[at], og_recv.at[at],
        )
        for at in range(pairs)
    ]

    def start_all(copies):
        for copy in copies:
            copy.start()

    def square_copies(mat):
        return [
            pltpu.make_async_remote_copy(
                src_ref=squares.at[mat],
                dst_ref=squares_got.at[mat, gap - 1],
                send_sem=sq_send.at[mat, gap - 1],
                recv_sem=sq_recv.at[mat, gap - 1],
                device_id=(me, tp_peer(gap)),
                device_id_type=mesh_ids,
            )
            for gap in range(1, tp_count)
        ]

    def put_squares(mat, tiles):
        total = jnp.zeros((8, 128), F32)
        for tile in tiles:
            squared = fold_rows(tile * tile, jnp.sum)
            for at in range(0, squared.shape[1], 128):
                total += squared[:, at : at + 128]
        squares[mat] = total
        start_all(square_copies(mat))

    entry_count = rank_share * fs_count * cols * tp_count

    def clip_of(mat):
        total = squares[mat]
        copies = square_copies(mat)
        for gap in range(1, tp_count):
            copies[gap - 1].wait_recv()
            total += squares_got[mat, gap - 1]
        total = jnp.sum(jnp.sum(total, axis=0, keepdims=True), axis=1, keepdims=True)
        return jnp.minimum(1.0, CLIP_RMS * math.sqrt(entry_count) / jnp.sqrt(total))

    place = jnp.where(me % 2 == 0, me // 2, fs_count - 1 - me // 2)

    def owner(at):
        at = lax.rem(at + 2 * fs_count, fs_count)
        return jnp.where(at < half_count, 2 * at, 2 * (fs_count - 1 - at) + 1)

    def halved(start, size, split):
        if split is None:
            return pl.ds(pl.multiple_of(start, size), size)
        return pl.ds(pl.multiple_of(start + split * (size // 2), size // 2), size // 2)

    def ring_block(mat, at, split):
        if mat == 0:
            return vcopy.at[halved(at * row_share, row_share, split)]
        rows = slice(None) if split is None else pl.ds(split * (cols // 2), cols // 2)
        return ocopy.at[rows, share(at, row_share)]

    def ring_copy(mat, step, way, arriving):
        back = step + 1 if arriving else step
        origin = owner(place - back if way == 0 else place + back)
        ref = ring_block(mat, origin, way if step == half_count - 1 else None)
        return pltpu.make_async_remote_copy(
            src_ref=ref,
            dst_ref=ref,
            send_sem=ring_send.at[mat, way, step],
            recv_sem=ring_recv.at[mat, way, step],
            device_id=(owner(place + 1 if way == 0 else place - 1), my_tp),
            device_id_type=mesh_ids,
        )

    def ring_begin(mat):
        for way in range(2):
            ring_copy(mat, 0, way, False).start()

    def ring_forward(mat, step):
        for way in range(2):
            ring_copy(mat, step, way, True).wait_recv()
            if step + 1 < half_count:
                ring_copy(mat, step + 1, way, False).start()

    def value_moments():
        for copy in late:
            copy.wait()
        proj = vproj[share(me, rank_share), :]
        for gap in range(1, fs_count):
            vscatter[gap - 1].wait_recv()
            proj += vgot[gap - 1]
        new_first, new_second, direction = moment_step(proj, vfirst[...], vsecond[...])
        vdirs[share(me, rank_share), :] = direction
        start_all(vgather)
        vfirst_new[...] = new_first
        vsecond_new[...] = new_second

    def value_squares():
        for copy in vgather:
            copy.wait_recv()
        put_squares(0, [vdirs[...]])
        high, low = split_two(vdirs[...])
        rows = vbasis_v[share(me, row_share), :]
        vstep[...] = dot_f32(rows, high) + dot_f32(rows, low)

    def value_update():
        step = clip_of(0) * vstep[...]
        vstep[...] = step
        weight = vweight[...] - LEARN_RATE * step
        vnew[...] = weight
        vcopy[share(me, row_share), :] = weight.astype(BF16)
        ring_begin(0)

    def out_moments(at):
        span = slice(at * wide, (at + 1) * wide)
        proj = oproj[at, share(me, rank_share), :]
        for gap in range(1, fs_count):
            oscatter[at][gap - 1].wait_recv()
            proj += ogot[at, gap - 1]
        new_first, new_second, direction = moment_step(proj, ofirst[:, span], osecond[:, span])
        odirs[at, share(me, rank_share), :] = direction
        start_all(ogather[at])
        ofirst_new[:, span] = new_first
        osecond_new[:, span] = new_second

    def out_arrived(at):
        for copy in ogather[at]:
            copy.wait_recv()

    def out_step(at):
        rows = obasis_v[share(me, row_share), :]
        high, low = split_two(odirs[at])
        ostep[at * wide : (at + 1) * wide, :] = dot_f32(high, rows, ((0,), (1,))) + dot_f32(
            low, rows, ((0,), (1,))
        )

    def out_update():
        put_squares(1, [odirs[at] for at in range(pairs)])
        out_step(pairs - 1)
        step = clip_of(1) * ostep[...]
        ostep[...] = step
        weight = oweight[...] - LEARN_RATE * step
        onew[...] = weight
        ocopy[:, share(me, row_share)] = weight.astype(BF16)
        ring_begin(1)

    start_all(vscatter)

    early[2].wait()
    obasis_t[...] = obasis_v[...].T

    def cot_block(at, carry):
        slot = lax.rem(at, SLOTS)
        chunk_copy(cot_h, at, slot).wait()
        high, low = split_two(dot_f32(obasis_t[...], chunks[slot], ((1,), (1,))))
        cb_high[at] = high
        cb_low[at] = low

        @pl.when(at < blocks - SLOTS)
        def _():
            chunk_copy(cot_h, at + SLOTS, slot).start()

        return carry

    lax.fori_loop(0, blocks, cot_block, 0)
    for copy in attention:
        copy.wait()
    for head in range(pairs * PAIR):
        value_t[head] = value_v[:, head * DV : (head + 1) * DV].T

    lane = lax.broadcasted_iota(jnp.int32, (TILE, DV), 1)

    def attend(block, pair, which):
        head = pair * PAIR + which
        columns = pl.ds(pl.multiple_of(head * DV, DV), DV)
        lam = lam_ref[head]
        width = (block + 1) * TILE
        query = query_v[block * TILE : (block + 1) * TILE, columns].astype(F32)
        query = query * (DH ** (-0.5) * LOG2E)
        parts_one = split_two(jnp.where(lane < DH, query, 0.0))
        parts_two = split_two(jnp.where(lane < DH, 0.0, query))
        query_one = jnp.concatenate(parts_one, axis=1)
        query_two = jnp.concatenate(parts_two, axis=1)
        peak_one = jnp.full((8, TILE), -jnp.inf, F32)
        peak_two = peak_one
        for at in range(0, width, TILE):
            keys = key_v[at : at + TILE, columns]
            keys = jnp.concatenate([keys, keys], axis=1)
            one = dot_f32(keys, query_one, ((1,), (1,)))
            two = dot_f32(keys, query_two, ((1,), (1,)))
            if at == width - TILE:
                one = one + tri[...]
                two = two + tri[...]
            score_one[at : at + TILE, :] = one
            score_two[at : at + TILE, :] = two
            peak_one = jnp.maximum(peak_one, fold_rows(one, jnp.max))
            peak_two = jnp.maximum(peak_two, fold_rows(two, jnp.max))
        peak_one = jnp.max(peak_one, axis=0, keepdims=True)
        peak_two = jnp.max(peak_two, axis=0, keepdims=True)
        sum_one = jnp.zeros((8, TILE), F32)
        sum_two = sum_one
        for at in range(0, width, TILE):
            one = jnp.exp2(score_one[at : at + TILE, :] - peak_one)
            two = jnp.exp2(score_two[at : at + TILE, :] - peak_two)
            score_one[at : at + TILE, :] = one
            score_two[at : at + TILE, :] = two
            sum_one += fold_rows(one, jnp.sum)
            sum_two += fold_rows(two, jnp.sum)
        rate_one = 1.0 / jnp.sum(sum_one, axis=0, keepdims=True)
        rate_two = lam / jnp.sum(sum_two, axis=0, keepdims=True)
        for at in range(0, width, TILE):
            mix_ref[at : at + TILE, :] = (
                score_one[at : at + TILE, :] * rate_one - score_two[at : at + TILE, :] * rate_two
            ).astype(BF16)
        raw = dot_f32(value_t[head, :, :width], mix_ref[:width, :])
        mean_sq = jnp.mean(raw * raw, axis=0, keepdims=True)
        gain = jnp.concatenate([gain_t[...]] * (TILE // DV), axis=1)
        out_t = (raw * lax.rsqrt(mean_sq + EPSILON_NORM) * gain).astype(BF16)
        span = slice(which * DV, (which + 1) * DV)
        oproj[pair, :, span] += dot_f32(cb_high[block], out_t, ((1,), (1,))) + dot_f32(
            cb_low[block], out_t, ((1,), (1,))
        )

    events = {}

    def plan(pair, item, action):
        events.setdefault((pair, item), []).append(action)

    last = 2 * blocks
    at = (8, 13, 14, 17, 21, 24, 27)
    actions = [value_moments, value_squares, value_update] + [
        functools.partial(ring_forward, 0, step) for step in range(half_count)
    ]
    for tick, action in zip(at, actions):
        plan(tick // last, tick % last, action)
    for pair in range(pairs - 1):
        plan(pair + 1, 2, functools.partial(start_all, oscatter[pair]))
        plan(pair + 1, 10, functools.partial(out_moments, pair))
        plan(pair + 1, 14, functools.partial(out_arrived, pair))
        plan(pair + 1, 14, functools.partial(out_step, pair))

    def pair_items(pair, carry):
        for item in range(last):
            for when in range(pairs):
                for action in events.get((when, item), []):
                    pl.when(pair == when)(action)
            attend(item // PAIR, pair, item % PAIR)
        return carry

    lax.fori_loop(0, pairs, pair_items, 0)
    start_all(oscatter[pairs - 1])
    for (pair, item) in sorted(events):
        if pair >= pairs:
            for action in events[(pair, item)]:
                action()
    out_moments(pairs - 1)
    out_arrived(pairs - 1)
    out_update()
    for step in range(half_count):
        ring_forward(1, step)
    for copy in vscatter + vgather + square_copies(0) + square_copies(1):
        copy.wait_send()
    for at in range(pairs):
        for copy in oscatter[at] + ogather[at]:
            copy.wait_send()
    for mat in range(2):
        for step in range(half_count):
            for way in range(2):
                ring_copy(mat, step, way, False).wait_send()


def body(
    query_rows, key_rows, value_rows, mix_lambda, head_gain, out_cotangent, layer_input,
    value_cotangent, out_weight, value_weight, out_basis, value_basis, out_first, out_second,
    value_first, value_second,
):
    fs_count = lax.axis_size("fs")
    tp_count = lax.axis_size("tp")
    seq_len, cols = query_rows.shape
    width, rank = out_basis.shape
    row_share = value_weight.shape[0]
    rank_share = rank // fs_count
    heads = mix_lambda.shape[0]
    pairs = heads // PAIR
    blocks = seq_len // TILE
    half_count = fs_count // 2
    dma = pltpu.SemaphoreType.DMA
    like = lambda a: jax.ShapeDtypeStruct(a.shape, a.dtype)
    vmem = lambda a: pltpu.VMEM(a.shape, a.dtype)
    anywhere = pl.BlockSpec(memory_space=pl.ANY)
    return pl.pallas_call(
        functools.partial(step_kernel, fs_count, tp_count),
        out_shape=(
            like(out_weight), like(value_weight), like(out_weight), like(value_weight),
            jax.ShapeDtypeStruct((cols, width), BF16),
            jax.ShapeDtypeStruct((width, cols), BF16),
            like(out_first), like(out_second), like(value_first), like(value_second),
        ),
        in_specs=[
            pl.BlockSpec(memory_space=pltpu.SMEM), pl.BlockSpec(memory_space=pltpu.VMEM),
        ] + [anywhere] * 14,
        out_specs=tuple([pl.BlockSpec(memory_space=pltpu.VMEM)] * 10),
        scratch_shapes=[
            vmem(query_rows), vmem(key_rows), vmem(value_rows), vmem(value_cotangent),
            vmem(out_basis), vmem(value_basis), vmem(out_weight), vmem(value_weight),
            vmem(out_first), vmem(out_second), vmem(value_first), vmem(value_second),
            pltpu.VMEM((SLOTS, TILE, width), BF16),
            pltpu.VMEM((seq_len, TILE), F32),
            pltpu.VMEM((seq_len, TILE), F32),
            pltpu.VMEM((seq_len, TILE), BF16),
            pltpu.VMEM((heads, DV, seq_len), BF16),
            pltpu.VMEM((rank, width), BF16),
            pltpu.VMEM((rank, width), BF16),
            pltpu.VMEM((blocks, rank, TILE), BF16),
            pltpu.VMEM((blocks, rank, TILE), BF16),
            pltpu.VMEM((DV, DV), F32),
            pltpu.VMEM((TILE, TILE), F32),
            pltpu.VMEM((rank, cols), F32),
            pltpu.VMEM((pairs, rank, PAIR * DV), F32),
            pltpu.VMEM((fs_count - 1, rank_share, cols), F32),
            pltpu.VMEM((pairs, fs_count - 1, rank_share, PAIR * DV), F32),
            pltpu.VMEM((rank, cols), F32),
            pltpu.VMEM((pairs, rank, PAIR * DV), F32),
            pltpu.VMEM((2, 8, 128), F32),
            pltpu.VMEM((2, tp_count - 1, 8, 128), F32),
            dma((12,)), dma((SLOTS,)),
            dma((fs_count - 1,)), dma((fs_count - 1,)),
            dma((pairs, fs_count - 1)), dma((pairs, fs_count - 1)),
            dma((fs_count - 1,)), dma((fs_count - 1,)),
            dma((pairs, fs_count - 1)), dma((pairs, fs_count - 1)),
            dma((2, tp_count - 1)), dma((2, tp_count - 1)),
            dma((2, 2, half_count)), dma((2, 2, half_count)),
        ],
        compiler_params=pltpu.CompilerParams(
            collective_id=0, has_side_effects=True, vmem_limit_bytes=62 * 1024 * 1024
        ),
        name="step",
    )(
        mix_lambda, head_gain.reshape(1, DV), query_rows, key_rows, value_rows, out_cotangent,
        layer_input, value_cotangent, out_basis, value_basis, out_weight, value_weight,
        out_first, out_second, value_first, value_second,
    )


def solution(mesh):
    placed = (
        P("fs", "tp"),
        P("fs", "tp"),
        P("fs", "tp"),
        P("tp"),
        P(),
        P("fs", None),
        P("fs", None),
        P("fs", "tp"),
        P("tp", "fs"),
        P("fs", "tp"),
        P(),
        P(),
        P("fs", "tp"),
        P("fs", "tp"),
        P("fs", "tp"),
        P("fs", "tp"),
    )
    return jax.shard_map(
        body,
        mesh=mesh,
        in_specs=placed,
        out_specs=(
            P("tp", "fs"),
            P("fs", "tp"),
            P("tp", "fs"),
            P("fs", "tp"),
            P("tp", None),
            P(None, "tp"),
            P("fs", "tp"),
            P("fs", "tp"),
            P("fs", "tp"),
            P("fs", "tp"),
        ),
        check_vma=False,
    )
```

```python
import functools
import math

import jax
import jax.numpy as jnp
from jax import lax
from jax.experimental import pallas as pl
from jax.experimental.pallas import tpu as pltpu
from jax.sharding import PartitionSpec as P

DH = 64
DV = 128


EPSILON_NORM = 1e-05
EPSILON_ADAM = 1e-08
BETA_ONE = 0.9
BETA_TWO = 0.95
CLIP_RMS = 1.0
LEARN_RATE = 0.01
TILE = 256
SLOTS = 4
EARLY = 4
PAIR = 2
LOG2E = 1.4426950408889634
F32 = jnp.float32
BF16 = jnp.bfloat16


def dot_f32(left, right, dims=((1,), (0,))):
    return lax.dot_general(left, right, (dims, ((), ())), preferred_element_type=F32)


def split_two(wide):
    high = wide.astype(BF16)
    return high, (wide - high.astype(F32)).astype(BF16)


def fold_rows(tile, op):
    rows, cols = tile.shape
    return op(tile.reshape(rows // 8, 8, cols), axis=0)


def moment_step(proj, first, second):
    new_first = BETA_ONE * first + (1.0 - BETA_ONE) * proj
    new_second = BETA_TWO * second + (1.0 - BETA_TWO) * proj * proj
    direction = new_first / (jnp.sqrt(new_second) + EPSILON_ADAM)
    return (new_first, new_second, direction)


def step_kernel(
    fs_count, tp_count,
    lam_ref, gain_ref, query_h, key_h, value_h, cot_h, input_h, vcot_h, obasis_h, vbasis_h,
    oweight_h, vweight_h, ofirst_h, osecond_h, vfirst_h, vsecond_h,
    vproj_o, oproj_o, vdirs_o, odirs_o, clips_o, vcopy_o, ocopy_o, early_o,
    query_v, key_v, value_v, vcot_v, obasis_v, vbasis_v, oweight, vweight,
    ofirst, osecond, vfirst, vsecond, chunks, vstep, ostep, vcopy, ocopy, early_w, clips,
    score_one, score_two, mix_ref, value_t, obasis_t, vbasis_t, cb_high, cb_low, gain_t, tri,
    vproj, oproj, vgot, ogot, vdirs, odirs, squares, squares_got,
    load_sem, chunk_sem, vs_send, vs_recv, os_send, os_recv, vg_send, vg_recv, og_send, og_recv,
    sq_send, sq_recv, ring_send, ring_recv, out_sem, block_sem,
):
    me = lax.axis_index("fs")
    my_tp = lax.axis_index("tp")
    half_count = fs_count // 2
    rank_share, cols = ofirst.shape
    row_share = vweight.shape[0]
    seq_len = query_v.shape[0]
    blocks = seq_len // TILE
    pairs = oproj.shape[0]
    wide = PAIR * DV
    early_rows = early_w.shape[0]
    mesh_ids = pl.DeviceIdType.MESH

    def fs_peer(gap):
        return lax.rem(me + gap, fs_count)

    def tp_peer(gap):
        return lax.rem(my_tp + gap, tp_count)

    def share(index, size):
        return pl.ds(pl.multiple_of(index * size, size), size)

    barrier = pltpu.get_barrier_semaphore()
    for gap in range(1, fs_count):
        pl.semaphore_signal(
            barrier, inc=1, device_id=(fs_peer(gap), my_tp), device_id_type=mesh_ids
        )
    for gap in range(1, tp_count):
        pl.semaphore_signal(
            barrier, inc=1, device_id=(me, tp_peer(gap)), device_id_type=mesh_ids
        )

    def chunk_copy(source, at, slot):
        return pltpu.make_async_copy(
            source.at[share(at, TILE)], chunks.at[slot], chunk_sem.at[slot]
        )

    def load(index, source, target):
        copy = pltpu.make_async_copy(source, target, load_sem.at[index])
        copy.start()
        return copy

    early = [load(0, vbasis_h, vbasis_v)]
    for at in range(SLOTS - 1):
        chunk_copy(input_h, at, at).start()
    early.append(load(1, vcot_h, vcot_v))
    chunk_copy(input_h, SLOTS - 1, SLOTS - 1).start()
    early.append(load(2, obasis_h, obasis_v))
    early_own = load(
        12, oweight_h.at[pl.ds(0, early_rows)], early_w.at[:, share(me, row_share)]
    )
    later = [
        (3, query_h, query_v), (4, key_h, key_v), (5, value_h, value_v),
        (6, vfirst_h, vfirst), (7, vsecond_h, vsecond), (8, ofirst_h, ofirst),
        (9, osecond_h, osecond), (10, vweight_h, vweight), (11, oweight_h, oweight),
    ]
    later = [
        pltpu.make_async_copy(source, target, load_sem.at[index])
        for index, source, target in later
    ]
    attention, late = later[:3], later[3:]

    key_pos = lax.broadcasted_iota(jnp.int32, (TILE, TILE), 0)
    query_pos = lax.broadcasted_iota(jnp.int32, (TILE, TILE), 1)
    tri[...] = jnp.where(key_pos <= query_pos, 0.0, -jnp.inf)
    gain_t[...] = jnp.broadcast_to(gain_ref[...], (DV, DV)).T
    vproj[...] = jnp.zeros_like(vproj)
    oproj[...] = jnp.zeros_like(oproj)

    def exchange(source, target, send, recv):
        copies = []
        for gap in range(1, fs_count):
            peer = fs_peer(gap)
            copies.append(
                pltpu.make_async_remote_copy(
                    src_ref=source(peer),
                    dst_ref=target(gap),
                    send_sem=send.at[gap - 1],
                    recv_sem=recv.at[gap - 1],
                    device_id=(peer, my_tp),
                    device_id_type=mesh_ids,
                )
            )
        return copies

    vscatter = exchange(
        lambda peer: vproj.at[share(peer, rank_share)], lambda gap: vgot.at[gap - 1],
        vs_send, vs_recv,
    )
    vgather = exchange(
        lambda peer: vdirs.at[share(me, rank_share)],
        lambda gap: vdirs.at[share(me, rank_share)], vg_send, vg_recv,
    )
    oscatter = [
        exchange(
            lambda peer, at=at: oproj.at[at, share(peer, rank_share)],
            lambda gap, at=at: ogot.at[at, gap - 1], os_send.at[at], os_recv.at[at],
        )
        for at in range(pairs)
    ]
    ogather = [
        exchange(
            lambda peer, at=at: odirs.at[at, share(me, rank_share)],
            lambda gap, at=at: odirs.at[at, share(me, rank_share)],
            og_send.at[at], og_recv.at[at],
        )
        for at in range(pairs)
    ]

    def start_all(copies):
        for copy in copies:
            copy.start()

    def square_copies(mat):
        return [
            pltpu.make_async_remote_copy(
                src_ref=squares.at[mat],
                dst_ref=squares_got.at[mat, gap - 1],
                send_sem=sq_send.at[mat, gap - 1],
                recv_sem=sq_recv.at[mat, gap - 1],
                device_id=(me, tp_peer(gap)),
                device_id_type=mesh_ids,
            )
            for gap in range(1, tp_count)
        ]

    def put_squares(mat, tiles):
        total = jnp.zeros((8, 128), F32)
        for tile in tiles:
            squared = fold_rows(tile * tile, jnp.sum)
            for at in range(0, squared.shape[1], 128):
                total += squared[:, at : at + 128]
        squares[mat] = total
        start_all(square_copies(mat))

    entry_count = rank_share * fs_count * cols * tp_count

    def clip_of(mat):
        total = squares[mat]
        copies = square_copies(mat)
        for gap in range(1, tp_count):
            copies[gap - 1].wait_recv()
            total += squares_got[mat, gap - 1]
        total = jnp.sum(jnp.sum(total, axis=0, keepdims=True), axis=1, keepdims=True)
        return jnp.minimum(1.0, CLIP_RMS * math.sqrt(entry_count) / jnp.sqrt(total))

    place = jnp.where(me % 2 == 0, me // 2, fs_count - 1 - me // 2)

    def owner(at):
        at = lax.rem(at + 2 * fs_count, fs_count)
        return jnp.where(at < half_count, 2 * at, 2 * (fs_count - 1 - at) + 1)

    def halved(start, size, split):
        if split is None:
            return pl.ds(pl.multiple_of(start, size), size)
        return pl.ds(pl.multiple_of(start + split * (size // 2), size // 2), size // 2)

    def ring_block(mat, at, split):
        if mat == 0:
            return vcopy.at[halved(at * row_share, row_share, split)]
        held = ocopy if mat == 1 else early_w
        count = held.shape[0]
        rows = slice(None) if split is None else pl.ds(split * (count // 2), count // 2)
        return held.at[rows, share(at, row_share)]

    def ring_copy(mat, step, way, arriving):
        back = step + 1 if arriving else step
        origin = owner(place - back if way == 0 else place + back)
        ref = ring_block(mat, origin, way if step == half_count - 1 else None)
        return pltpu.make_async_remote_copy(
            src_ref=ref,
            dst_ref=ref,
            send_sem=ring_send.at[mat, way, step],
            recv_sem=ring_recv.at[mat, way, step],
            device_id=(owner(place + 1 if way == 0 else place - 1), my_tp),
            device_id_type=mesh_ids,
        )

    def ring_begin(mat):
        for way in range(2):
            ring_copy(mat, 0, way, False).start()

    def ring_forward(mat, step):
        for way in range(2):
            ring_copy(mat, step, way, True).wait_recv()
            if step + 1 < half_count:
                ring_copy(mat, step + 1, way, False).start()

    sends = [
        (vproj.at[share(me, rank_share)], vproj_o), (vdirs, vdirs_o),
    ]
    for at in range(pairs):
        sends += [
            (oproj.at[at, share(me, rank_share)], oproj_o.at[at]), (odirs.at[at], odirs_o.at[at]),
        ]
    sends += [(clips, clips_o), (vcopy, vcopy_o), (early_w, early_o)]

    def out_copy(index):
        source, target = sends[index]
        return pltpu.make_async_copy(source, target, out_sem.at[index])

    def block_copy(at):
        columns = share(at, row_share)
        return pltpu.make_async_copy(
            ocopy.at[:, columns], ocopy_o.at[:, columns], block_sem.at[at]
        )

    def value_moments():
        for copy in late:
            copy.wait()
        proj = vproj[share(me, rank_share), :]
        for gap in range(1, fs_count):
            vscatter[gap - 1].wait_recv()
            proj += vgot[gap - 1]
        direction = moment_step(proj, vfirst[...], vsecond[...])[2]
        vdirs[share(me, rank_share), :] = direction
        start_all(vgather)
        vproj[share(me, rank_share), :] = proj
        out_copy(0).start()

    def value_squares():
        for copy in vgather:
            copy.wait_recv()
        put_squares(0, [vdirs[...]])
        out_copy(1).start()
        high, low = split_two(vdirs[...])
        rows = vbasis_v[share(me, row_share), :]
        vstep[...] = dot_f32(rows, high) + dot_f32(rows, low)

    def value_update():
        clip = clip_of(0)
        clips[0] = jnp.broadcast_to(clip, (8, 128))
        weight = vweight[...] - LEARN_RATE * (clip * vstep[...])
        vcopy[share(me, row_share), :] = weight.astype(BF16)
        ring_begin(0)

    def out_moments(at):
        span = slice(at * wide, (at + 1) * wide)
        proj = oproj[at, share(me, rank_share), :]
        for gap in range(1, fs_count):
            oscatter[at][gap - 1].wait_recv()
            proj += ogot[at, gap - 1]
        direction = moment_step(proj, ofirst[:, span], osecond[:, span])[2]
        odirs[at, share(me, rank_share), :] = direction
        start_all(ogather[at])
        oproj[at, share(me, rank_share), :] = proj
        out_copy(2 + 2 * at).start()

    def out_arrived(at):
        for copy in ogather[at]:
            copy.wait_recv()
        out_copy(3 + 2 * at).start()

    def out_step(at):
        rows = obasis_v[share(me, row_share), :]
        high, low = split_two(odirs[at])
        ostep[at * wide : (at + 1) * wide, :] = dot_f32(high, rows, ((0,), (1,))) + dot_f32(
            low, rows, ((0,), (1,))
        )

    def out_update():
        put_squares(1, [odirs[at] for at in range(pairs)])
        out_step(pairs - 1)
        clip = clip_of(1)
        clips[1] = jnp.broadcast_to(clip, (8, 128))
        rows = pl.ds(early_rows, cols - early_rows)
        weight = oweight[rows, :] - LEARN_RATE * (clip * ostep[rows, :])
        ocopy[:, share(me, row_share)] = weight.astype(BF16)
        ring_begin(1)
        out_copy(2 + 2 * pairs).start()
        block_copy(me).start()

    def enter():
        pl.semaphore_wait(barrier, fs_count + tp_count - 2)
        early_own.wait()
        ring_begin(2)

    early[0].wait()
    vbasis_t[...] = vbasis_v[...].T
    early[1].wait()

    def value_block(at, carry):
        slot = lax.rem(at, SLOTS)
        chunk_copy(input_h, at, slot).wait()
        high, low = split_two(dot_f32(vbasis_t[...], chunks[slot], ((1,), (1,))))
        vcot = vcot_v[share(at, TILE), :]
        vproj[...] += dot_f32(high, vcot) + dot_f32(low, vcot)

        @pl.when(at < blocks - SLOTS)
        def _():
            chunk_copy(input_h, at + SLOTS, slot).start()

        @pl.when(at >= blocks - SLOTS)
        def _():
            chunk_copy(cot_h, at - (blocks - SLOTS), slot).start()

        @pl.when(at == SLOTS)
        def _():
            start_all(later)

        pl.when(at == 2)(enter)
        return carry

    lax.fori_loop(0, blocks, value_block, 0)
    start_all(vscatter)

    early[2].wait()
    obasis_t[...] = obasis_v[...].T

    def cot_block(at, carry):
        slot = lax.rem(at, SLOTS)
        chunk_copy(cot_h, at, slot).wait()
        high, low = split_two(dot_f32(obasis_t[...], chunks[slot], ((1,), (1,))))
        cb_high[at] = high
        cb_low[at] = low

        @pl.when(at < blocks - SLOTS)
        def _():
            chunk_copy(cot_h, at + SLOTS, slot).start()

        return carry

    lax.fori_loop(0, blocks, cot_block, 0)
    ring_forward(2, 0)
    for copy in attention:
        copy.wait()
    for head in range(pairs * PAIR):
        value_t[head] = value_v[:, head * DV : (head + 1) * DV].T

    lane = lax.broadcasted_iota(jnp.int32, (TILE, DV), 1)

    def attend(block, pair, which):
        head = pair * PAIR + which
        columns = pl.ds(pl.multiple_of(head * DV, DV), DV)
        lam = lam_ref[head]
        width = (block + 1) * TILE
        query = query_v[block * TILE : (block + 1) * TILE, columns].astype(F32)
        query = query * (DH ** (-0.5) * LOG2E)
        parts_one = split_two(jnp.where(lane < DH, query, 0.0))
        parts_two = split_two(jnp.where(lane < DH, 0.0, query))
        query_one = jnp.concatenate(parts_one, axis=1)
        query_two = jnp.concatenate(parts_two, axis=1)
        peak_one = jnp.full((8, TILE), -jnp.inf, F32)
        peak_two = peak_one
        for at in range(0, width, TILE):
            keys = key_v[at : at + TILE, columns]
            keys = jnp.concatenate([keys, keys], axis=1)
            one = dot_f32(keys, query_one, ((1,), (1,)))
            two = dot_f32(keys, query_two, ((1,), (1,)))
            if at == width - TILE:
                one = one + tri[...]
                two = two + tri[...]
            score_one[at : at + TILE, :] = one
            score_two[at : at + TILE, :] = two
            peak_one = jnp.maximum(peak_one, fold_rows(one, jnp.max))
            peak_two = jnp.maximum(peak_two, fold_rows(two, jnp.max))
        peak_one = jnp.max(peak_one, axis=0, keepdims=True)
        peak_two = jnp.max(peak_two, axis=0, keepdims=True)
        sum_one = jnp.zeros((8, TILE), F32)
        sum_two = sum_one
        for at in range(0, width, TILE):
            one = jnp.exp2(score_one[at : at + TILE, :] - peak_one)
            two = jnp.exp2(score_two[at : at + TILE, :] - peak_two)
            score_one[at : at + TILE, :] = one
            score_two[at : at + TILE, :] = two
            sum_one += fold_rows(one, jnp.sum)
            sum_two += fold_rows(two, jnp.sum)
        rate_one = 1.0 / jnp.sum(sum_one, axis=0, keepdims=True)
        rate_two = lam / jnp.sum(sum_two, axis=0, keepdims=True)
        for at in range(0, width, TILE):
            mix_ref[at : at + TILE, :] = (
                score_one[at : at + TILE, :] * rate_one - score_two[at : at + TILE, :] * rate_two
            ).astype(BF16)
        raw = dot_f32(value_t[head, :, :width], mix_ref[:width, :])
        mean_sq = jnp.mean(raw * raw, axis=0, keepdims=True)
        gain = jnp.concatenate([gain_t[...]] * (TILE // DV), axis=1)
        out_t = (raw * lax.rsqrt(mean_sq + EPSILON_NORM) * gain).astype(BF16)
        span = slice(which * DV, (which + 1) * DV)
        oproj[pair, :, span] += dot_f32(cb_high[block], out_t, ((1,), (1,))) + dot_f32(
            cb_low[block], out_t, ((1,), (1,))
        )

    events = {}

    def plan(pair, item, action):
        events.setdefault((pair, item), []).append(action)

    last = 2 * blocks
    at = (11, 17, 19, 26, 30)
    actions = [value_moments, value_squares, value_update] + [
        functools.partial(ring_forward, 0, step) for step in range(2)
    ]

    def early_done():
        for step in range(3, half_count):
            ring_forward(2, step)
        out_copy(4 + 2 * pairs).start()

    plan(0, 8, functools.partial(ring_forward, 2, 1))
    plan(0, 12, functools.partial(ring_forward, 2, 2))
    plan(0, 15, early_done)
    for tick, action in zip(at, actions):
        plan(tick // last, tick % last, action)
    for pair in range(pairs - 1):
        plan(pair + 1, 0, functools.partial(start_all, oscatter[pair]))
        plan(pair + 1, 8, functools.partial(out_moments, pair))
        plan(pair + 1, 15, functools.partial(out_arrived, pair))
        plan(pair + 1, 15, functools.partial(out_step, pair))

    def pair_items(pair, carry):
        for item in range(last):
            for when in range(pairs):
                for action in events.get((when, item), []):
                    pl.when(pair == when)(action)
            attend(item // PAIR, pair, item % PAIR)
        return carry

    lax.fori_loop(0, pairs, pair_items, 0)
    start_all(oscatter[pairs - 1])
    for (pair, item) in sorted(events):
        if pair >= pairs:
            for action in events[(pair, item)]:
                action()
    for step in range(2, half_count - 1):
        ring_forward(0, step)
    out_moments(pairs - 1)
    ring_forward(0, half_count - 1)
    out_copy(3 + 2 * pairs).start()
    out_arrived(pairs - 1)
    out_update()
    for step in range(half_count):
        ring_forward(1, step)
        back = step + 1
        if step < half_count - 1:
            block_copy(owner(place - back)).start()
        block_copy(owner(place + back)).start()
    for copy in vscatter + vgather + square_copies(0) + square_copies(1):
        copy.wait_send()
    for at in range(pairs):
        for copy in oscatter[at] + ogather[at]:
            copy.wait_send()
    for mat in range(3):
        for step in range(half_count):
            for way in range(2):
                ring_copy(mat, step, way, False).wait_send()
    for index in range(len(sends)):
        out_copy(index).wait()
    for at in range(fs_count):
        block_copy(at).wait()


def finish_kernel(*refs):
    inputs, outputs, scratch = refs[:16], refs[16:26], refs[26:]
    in_sem, out_sem = scratch[-2:]
    held, results, early_copy = scratch[:16], scratch[16:24], scratch[24]
    (
        clips, vproj, oproj, ofirst, osecond, vfirst, vsecond, vdirs, odirs, obasis, vbasis,
        oweight, vweight, early_w, vcopy, ocopy,
    ) = held
    (
        ostep_o, vstep_o, onew_o, vnew_o, ocopy_o, vcopy_o, ofirst_o, osecond_o, vfirst_o,
        vsecond_o,
    ) = outputs
    ostep, vstep, onew, vnew, ofirst_new, osecond_new, vfirst_new, vsecond_new = results
    me = lax.axis_index("fs")
    row_share = vweight.shape[0]
    rows = pl.ds(pl.multiple_of(me * row_share, row_share), row_share)
    early_rows = early_w.shape[0]
    arrivals = [
        pltpu.make_async_copy(source, target, in_sem.at[index])
        for index, (source, target) in enumerate(zip(inputs, held))
    ]
    for copy in arrivals:
        copy.start()
    leaving = []

    def leave(source, target):
        copy = pltpu.make_async_copy(source, target, out_sem.at[len(leaving)])
        copy.start()
        leaving.append(copy)

    for index in range(14):
        arrivals[index].wait()
    clip_value = clips[0, :1, :1]
    clip_out = clips[1, :1, :1]
    pairs, rank, wide = odirs.shape
    out_parts = [split_two(odirs[at]) for at in range(pairs)]
    for start in range(0, early_rows, wide):
        count = min(wide, early_rows - start)
        high, low = out_parts[start // wide]
        high, low = high[:, :count], low[:, :count]
        step = dot_f32(high, obasis[...], ((0,), (1,))) + dot_f32(low, obasis[...], ((0,), (1,)))
        span = slice(start, start + count)
        early_copy[span, :] = (early_w[span, :] - LEARN_RATE * (clip_out * step)).astype(BF16)
    leave(early_copy, ocopy_o.at[pl.ds(0, early_rows)])
    arrivals[14].wait()
    leave(vcopy, vcopy_o)
    arrivals[15].wait()
    leave(ocopy, ocopy_o.at[pl.ds(early_rows, ocopy.shape[0])])
    high, low = split_two(vdirs[...])
    step = clip_value * (dot_f32(vbasis[rows, :], high) + dot_f32(vbasis[rows, :], low))
    vstep[...] = step
    leave(vstep, vstep_o)
    vnew[...] = vweight[...] - LEARN_RATE * step
    leave(vnew, vnew_o)
    for at in range(pairs):
        high, low = out_parts[at]
        step = clip_out * (
            dot_f32(high, obasis[rows, :], ((0,), (1,)))
            + dot_f32(low, obasis[rows, :], ((0,), (1,)))
        )
        span = slice(at * wide, (at + 1) * wide)
        ostep[span, :] = step
        onew[span, :] = oweight[span, :] - LEARN_RATE * step
        moments = moment_step(oproj[at], ofirst[:, span], osecond[:, span])
        ofirst_new[:, span] = moments[0]
        osecond_new[:, span] = moments[1]
    moments = moment_step(vproj[...], vfirst[...], vsecond[...])
    vfirst_new[...] = moments[0]
    vsecond_new[...] = moments[1]
    leave(ostep, ostep_o)
    leave(onew, onew_o)
    leave(ofirst_new, ofirst_o)
    leave(osecond_new, osecond_o)
    leave(vfirst_new, vfirst_o)
    leave(vsecond_new, vsecond_o)
    for copy in leaving:
        copy.wait()


def body(
    query_rows, key_rows, value_rows, mix_lambda, head_gain, out_cotangent, layer_input,
    value_cotangent, out_weight, value_weight, out_basis, value_basis, out_first, out_second,
    value_first, value_second,
):
    fs_count = lax.axis_size("fs")
    tp_count = lax.axis_size("tp")
    seq_len, cols = query_rows.shape
    width, rank = out_basis.shape
    row_share = value_weight.shape[0]
    rank_share = rank // fs_count
    heads = mix_lambda.shape[0]
    pairs = heads // PAIR
    blocks = seq_len // TILE
    half_count = fs_count // 2
    dma = pltpu.SemaphoreType.DMA
    like = lambda a: jax.ShapeDtypeStruct(a.shape, a.dtype)
    vmem = lambda a: pltpu.VMEM(a.shape, a.dtype)
    anywhere = pl.BlockSpec(memory_space=pl.ANY)
    early_rows = cols // EARLY
    early_shape = (early_rows, width)
    rest_shape = (cols - early_rows, width)
    vproj, oproj, vdirs, odirs, clips, vcopy, ocopy, early_w = pl.pallas_call(
        functools.partial(step_kernel, fs_count, tp_count),
        out_shape=(
            like(value_first),
            jax.ShapeDtypeStruct((pairs, rank_share, PAIR * DV), F32),
            jax.ShapeDtypeStruct((rank, cols), F32),
            jax.ShapeDtypeStruct((pairs, rank, PAIR * DV), F32),
            jax.ShapeDtypeStruct((2, 8, 128), F32),
            jax.ShapeDtypeStruct((width, cols), BF16),
            jax.ShapeDtypeStruct(rest_shape, BF16),
            jax.ShapeDtypeStruct(early_shape, F32),
        ),
        in_specs=[
            pl.BlockSpec(memory_space=pltpu.SMEM), pl.BlockSpec(memory_space=pltpu.VMEM),
        ] + [anywhere] * 14,
        out_specs=tuple([anywhere] * 8),
        scratch_shapes=[
            vmem(query_rows), vmem(key_rows), vmem(value_rows), vmem(value_cotangent),
            vmem(out_basis), vmem(value_basis), vmem(out_weight), vmem(value_weight),
            vmem(out_first), vmem(out_second), vmem(value_first), vmem(value_second),
            pltpu.VMEM((SLOTS, TILE, width), BF16),
            vmem(value_weight), vmem(out_weight), pltpu.VMEM((width, cols), BF16),
            pltpu.VMEM(rest_shape, BF16), pltpu.VMEM(early_shape, F32),
            pltpu.VMEM((2, 8, 128), F32),
            pltpu.VMEM((seq_len, TILE), F32),
            pltpu.VMEM((seq_len, TILE), F32),
            pltpu.VMEM((seq_len, TILE), BF16),
            pltpu.VMEM((heads, DV, seq_len), BF16),
            pltpu.VMEM((rank, width), BF16),
            pltpu.VMEM((rank, width), BF16),
            pltpu.VMEM((blocks, rank, TILE), BF16),
            pltpu.VMEM((blocks, rank, TILE), BF16),
            pltpu.VMEM((DV, DV), F32),
            pltpu.VMEM((TILE, TILE), F32),
            pltpu.VMEM((rank, cols), F32),
            pltpu.VMEM((pairs, rank, PAIR * DV), F32),
            pltpu.VMEM((fs_count - 1, rank_share, cols), F32),
            pltpu.VMEM((pairs, fs_count - 1, rank_share, PAIR * DV), F32),
            pltpu.VMEM((rank, cols), F32),
            pltpu.VMEM((pairs, rank, PAIR * DV), F32),
            pltpu.VMEM((2, 8, 128), F32),
            pltpu.VMEM((2, tp_count - 1, 8, 128), F32),
            dma((13,)), dma((SLOTS,)),
            dma((fs_count - 1,)), dma((fs_count - 1,)),
            dma((pairs, fs_count - 1)), dma((pairs, fs_count - 1)),
            dma((fs_count - 1,)), dma((fs_count - 1,)),
            dma((pairs, fs_count - 1)), dma((pairs, fs_count - 1)),
            dma((2, tp_count - 1)), dma((2, tp_count - 1)),
            dma((3, 2, half_count)), dma((3, 2, half_count)),
            dma((5 + 2 * pairs,)), dma((fs_count,)),
        ],
        compiler_params=pltpu.CompilerParams(
            collective_id=0, has_side_effects=True, vmem_limit_bytes=62 * 1024 * 1024
        ),
        name="step",
    )(
        mix_lambda, head_gain.reshape(1, DV), query_rows, key_rows, value_rows, out_cotangent,
        layer_input, value_cotangent, out_basis, value_basis, out_weight, value_weight,
        out_first, out_second, value_first, value_second,
    )
    results = (
        like(out_weight), like(value_weight), like(out_weight), like(value_weight),
        jax.ShapeDtypeStruct((cols, width), BF16),
        jax.ShapeDtypeStruct((width, cols), BF16),
        like(out_first), like(out_second), like(value_first), like(value_second),
    )
    operands = (
        clips, vproj, oproj, out_first, out_second, value_first, value_second, vdirs, odirs,
        out_basis, value_basis, out_weight, value_weight, early_w, vcopy, ocopy,
    )
    return pl.pallas_call(
        finish_kernel,
        out_shape=results,
        in_specs=[anywhere] * len(operands),
        out_specs=tuple([anywhere] * len(results)),
        scratch_shapes=[vmem(a) for a in operands + results[:4] + results[6:]] + [
            pltpu.VMEM(early_shape, BF16), dma((len(operands),)), dma((11,)),
        ],
        compiler_params=pltpu.CompilerParams(vmem_limit_bytes=62 * 1024 * 1024),
        name="finish",
    )(*operands)


def solution(mesh):
    placed = (
        P("fs", "tp"),
        P("fs", "tp"),
        P("fs", "tp"),
        P("tp"),
        P(),
        P("fs", None),
        P("fs", None),
        P("fs", "tp"),
        P("tp", "fs"),
        P("fs", "tp"),
        P(),
        P(),
        P("fs", "tp"),
        P("fs", "tp"),
        P("fs", "tp"),
        P("fs", "tp"),
    )
    return jax.shard_map(
        body,
        mesh=mesh,
        in_specs=placed,
        out_specs=(
            P("tp", "fs"),
            P("fs", "tp"),
            P("tp", "fs"),
            P("fs", "tp"),
            P("tp", None),
            P(None, "tp"),
            P("fs", "tp"),
            P("fs", "tp"),
            P("fs", "tp"),
            P("fs", "tp"),
        ),
        check_vma=False,
    )
```

```python
import functools
import math

import jax
import jax.numpy as jnp
from jax import lax
from jax.experimental import pallas as pl
from jax.experimental.pallas import tpu as pltpu
from jax.sharding import PartitionSpec as P

DH = 64
DV = 128


EPSILON_NORM = 1e-05
EPSILON_ADAM = 1e-08
BETA_ONE = 0.9
BETA_TWO = 0.95
CLIP_RMS = 1.0
LEARN_RATE = 0.01
TILE = 256
SLOTS = 4
EARLY = 8
HELD = 4
PAIR = 2
LOG2E = 1.4426950408889634
F32 = jnp.float32
BF16 = jnp.bfloat16


def dot_f32(left, right, dims=((1,), (0,))):
    return lax.dot_general(left, right, (dims, ((), ())), preferred_element_type=F32)


def split_two(wide):
    high = wide.astype(BF16)
    return high, (wide - high.astype(F32)).astype(BF16)


def fold_rows(tile, op):
    rows, cols = tile.shape
    return op(tile.reshape(rows // 8, 8, cols), axis=0)


def moment_step(proj, first, second):
    new_first = BETA_ONE * first + (1.0 - BETA_ONE) * proj
    new_second = BETA_TWO * second + (1.0 - BETA_TWO) * proj * proj
    direction = new_first / (jnp.sqrt(new_second) + EPSILON_ADAM)
    return (new_first, new_second, direction)


def step_kernel(
    fs_count, tp_count,
    lam_ref, gain_ref, query_h, key_h, value_h, cot_h, input_h, vcot_h, obasis_h, vbasis_h,
    oweight_h, vweight_h, ofirst_h, osecond_h, vfirst_h, vsecond_h,
    vproj_o, oproj_o, vdirs_o, odirs_o, clips_o, vcopy_o, ocopy_o, early_o,
    query_v, key_v, value_v, vcot_v, obasis_v, vbasis_v, oweight, vweight,
    ofirst, osecond, vfirst, vsecond, chunks, vstep, ostep, vcopy, ocopy, early_w, clips,
    scores, peak_ref, sum_ref, mix_ref, value_t, obasis_t, vbasis_t, cb_high, cb_low, gain_t, tri,
    vproj, oproj, vgot, ogot, vdirs, odirs, squares, squares_got,
    load_sem, chunk_sem, vs_send, vs_recv, os_send, os_recv,
    sq_send, sq_recv, ring_send, ring_recv, out_sem, block_sem,
):
    me = lax.axis_index("fs")
    my_tp = lax.axis_index("tp")
    half_count = fs_count // 2
    rank_share, cols = ofirst.shape
    row_share = vweight.shape[0]
    seq_len = query_v.shape[0]
    blocks = seq_len // TILE
    pairs = oproj.shape[0]
    wide = PAIR * DV
    early_rows = early_w.shape[0]
    mesh_ids = pl.DeviceIdType.MESH

    def fs_peer(gap):
        return lax.rem(me + gap, fs_count)

    def tp_peer(gap):
        return lax.rem(my_tp + gap, tp_count)

    def share(index, size):
        return pl.ds(pl.multiple_of(index * size, size), size)

    barrier = pltpu.get_barrier_semaphore()
    for gap in range(1, fs_count):
        pl.semaphore_signal(
            barrier, inc=1, device_id=(fs_peer(gap), my_tp), device_id_type=mesh_ids
        )
    for gap in range(1, tp_count):
        pl.semaphore_signal(
            barrier, inc=1, device_id=(me, tp_peer(gap)), device_id_type=mesh_ids
        )

    def chunk_copy(source, at, slot):
        return pltpu.make_async_copy(
            source.at[share(at, TILE)], chunks.at[slot], chunk_sem.at[slot]
        )

    def load(index, source, target):
        copy = pltpu.make_async_copy(source, target, load_sem.at[index])
        copy.start()
        return copy

    early = [load(0, vbasis_h, vbasis_v)]
    for at in range(SLOTS - 1):
        chunk_copy(input_h, at, at).start()
    early.append(load(1, vcot_h, vcot_v))
    chunk_copy(input_h, SLOTS - 1, SLOTS - 1).start()
    early.append(load(2, obasis_h, obasis_v))
    early_own = load(
        12, oweight_h.at[pl.ds(0, early_rows)], early_w.at[:, share(me, row_share)]
    )
    later = [
        (3, query_h, query_v), (4, key_h, key_v), (5, value_h, value_v),
        (6, vfirst_h, vfirst), (7, vsecond_h, vsecond), (8, ofirst_h, ofirst),
        (9, osecond_h, osecond), (10, vweight_h, vweight), (11, oweight_h, oweight),
    ]
    later = [
        pltpu.make_async_copy(source, target, load_sem.at[index])
        for index, source, target in later
    ]
    attention, late = later[:3], later[3:]

    key_pos = lax.broadcasted_iota(jnp.int32, (TILE, TILE), 0)
    query_pos = lax.broadcasted_iota(jnp.int32, (TILE, TILE), 1)
    tri[...] = jnp.where(key_pos <= query_pos, 0.0, -jnp.inf)
    gain_t[...] = jnp.broadcast_to(gain_ref[...], (DV, DV)).T
    vproj[...] = jnp.zeros_like(vproj)
    oproj[...] = jnp.zeros_like(oproj)

    def exchange(source, target, send, recv):
        copies = []
        for gap in range(1, fs_count):
            peer = fs_peer(gap)
            copies.append(
                pltpu.make_async_remote_copy(
                    src_ref=source(peer),
                    dst_ref=target(gap),
                    send_sem=send.at[gap - 1],
                    recv_sem=recv.at[gap - 1],
                    device_id=(peer, my_tp),
                    device_id_type=mesh_ids,
                )
            )
        return copies

    vscatter = exchange(
        lambda peer: vproj.at[share(peer, rank_share)], lambda gap: vgot.at[gap - 1],
        vs_send, vs_recv,
    )
    oscatter = [
        exchange(
            lambda peer, at=at: oproj.at[at, share(peer, rank_share)],
            lambda gap, at=at: ogot.at[at, gap - 1], os_send.at[at], os_recv.at[at],
        )
        for at in range(pairs)
    ]
    def start_all(copies):
        for copy in copies:
            copy.start()

    def square_copies(mat):
        return [
            pltpu.make_async_remote_copy(
                src_ref=squares.at[mat],
                dst_ref=squares_got.at[mat, gap - 1],
                send_sem=sq_send.at[mat, gap - 1],
                recv_sem=sq_recv.at[mat, gap - 1],
                device_id=(me, tp_peer(gap)),
                device_id_type=mesh_ids,
            )
            for gap in range(1, tp_count)
        ]

    def put_squares(mat, tiles):
        total = jnp.zeros((8, 128), F32)
        for tile in tiles:
            squared = fold_rows(tile * tile, jnp.sum)
            for at in range(0, squared.shape[1], 128):
                total += squared[:, at : at + 128]
        squares[mat] = total
        start_all(square_copies(mat))

    entry_count = rank_share * fs_count * cols * tp_count

    def clip_of(mat):
        total = squares[mat]
        copies = square_copies(mat)
        for gap in range(1, tp_count):
            copies[gap - 1].wait_recv()
            total += squares_got[mat, gap - 1]
        total = jnp.sum(jnp.sum(total, axis=0, keepdims=True), axis=1, keepdims=True)
        return jnp.minimum(1.0, CLIP_RMS * math.sqrt(entry_count) / jnp.sqrt(total))

    place = jnp.where(me % 2 == 0, me // 2, fs_count - 1 - me // 2)

    def owner(at):
        at = lax.rem(at + 2 * fs_count, fs_count)
        return jnp.where(at < half_count, 2 * at, 2 * (fs_count - 1 - at) + 1)

    def halved(start, size, split):
        if split is None:
            return pl.ds(pl.multiple_of(start, size), size)
        return pl.ds(pl.multiple_of(start + split * (size // 2), size // 2), size // 2)

    def ring_block(mat, at, split):
        if mat == 0:
            return vcopy.at[halved(at * row_share, row_share, split)]
        if mat == 3:
            return vdirs.at[halved(at * rank_share, rank_share, split)]
        if mat > 3:
            return odirs.at[mat - 4, halved(at * rank_share, rank_share, split)]
        held = ocopy if mat == 1 else early_w
        count = held.shape[0]
        rows = slice(None) if split is None else pl.ds(split * (count // 2), count // 2)
        return held.at[rows, share(at, row_share)]

    def ring_copy(mat, step, way, arriving):
        back = step + 1 if arriving else step
        origin = owner(place - back if way == 0 else place + back)
        ref = ring_block(mat, origin, way if step == half_count - 1 else None)
        return pltpu.make_async_remote_copy(
            src_ref=ref,
            dst_ref=ref,
            send_sem=ring_send.at[mat, way, step],
            recv_sem=ring_recv.at[mat, way, step],
            device_id=(owner(place + 1 if way == 0 else place - 1), my_tp),
            device_id_type=mesh_ids,
        )

    def ring_begin(mat):
        for way in range(2):
            ring_copy(mat, 0, way, False).start()

    def ring_forward(mat, step):
        for way in range(2):
            ring_copy(mat, step, way, True).wait_recv()
            if step + 1 < half_count:
                ring_copy(mat, step + 1, way, False).start()

    sends = [
        (vproj.at[share(me, rank_share)], vproj_o), (vdirs, vdirs_o),
    ]
    for at in range(pairs):
        sends += [
            (oproj.at[at, share(me, rank_share)], oproj_o.at[at]), (odirs.at[at], odirs_o.at[at]),
        ]
    sends += [(clips, clips_o), (vcopy, vcopy_o), (early_w, early_o)]

    def out_copy(index):
        source, target = sends[index]
        return pltpu.make_async_copy(source, target, out_sem.at[index])

    def block_copy(at):
        columns = share(at, row_share)
        return pltpu.make_async_copy(
            ocopy.at[:, columns], ocopy_o.at[:, columns], block_sem.at[at]
        )

    def value_moments():
        for copy in late:
            copy.wait()
        proj = vproj[share(me, rank_share), :]
        for gap in range(1, fs_count):
            vscatter[gap - 1].wait_recv()
            proj += vgot[gap - 1]
        direction = moment_step(proj, vfirst[...], vsecond[...])[2]
        vdirs[share(me, rank_share), :] = direction
        ring_begin(3)
        vproj[share(me, rank_share), :] = proj
        out_copy(0).start()

    def value_squares():
        for step in range(3, half_count):
            ring_forward(3, step)
        put_squares(0, [vdirs[...]])
        out_copy(1).start()
        high, low = split_two(vdirs[...])
        rows = vbasis_v[share(me, row_share), :]
        vstep[...] = dot_f32(rows, high) + dot_f32(rows, low)

    def value_update():
        clip = clip_of(0)
        clips[0] = jnp.broadcast_to(clip, (8, 128))
        weight = vweight[...] - LEARN_RATE * (clip * vstep[...])
        vcopy[share(me, row_share), :] = weight.astype(BF16)
        ring_begin(0)

    def out_moments(at):
        span = slice(at * wide, (at + 1) * wide)
        proj = oproj[at, share(me, rank_share), :]
        for gap in range(1, fs_count):
            oscatter[at][gap - 1].wait_recv()
            proj += ogot[at, gap - 1]
        direction = moment_step(proj, ofirst[:, span], osecond[:, span])[2]
        odirs[at, share(me, rank_share), :] = direction
        ring_begin(4 + at)
        oproj[at, share(me, rank_share), :] = proj
        out_copy(2 + 2 * at).start()

    def out_arrived(at):
        out_copy(3 + 2 * at).start()

    def out_step(at):
        rows = obasis_v[share(me, row_share), :]
        high, low = split_two(odirs[at])
        ostep[at * wide : (at + 1) * wide, :] = dot_f32(high, rows, ((0,), (1,))) + dot_f32(
            low, rows, ((0,), (1,))
        )

    def out_update():
        put_squares(1, [odirs[at] for at in range(pairs)])
        out_step(pairs - 1)
        clip = clip_of(1)
        clips[1] = jnp.broadcast_to(clip, (8, 128))
        rows = pl.ds(early_rows, cols - early_rows)
        weight = oweight[rows, :] - LEARN_RATE * (clip * ostep[rows, :])
        ocopy[:, share(me, row_share)] = weight.astype(BF16)
        ring_begin(1)
        out_copy(2 + 2 * pairs).start()
        block_copy(me).start()

    def enter():
        pl.semaphore_wait(barrier, fs_count + tp_count - 2)
        early_own.wait()
        ring_begin(2)

    early[0].wait()
    vbasis_t[...] = vbasis_v[...].T
    early[1].wait()

    def value_block(at, carry):
        slot = lax.rem(at, SLOTS)
        chunk_copy(input_h, at, slot).wait()
        high, low = split_two(dot_f32(vbasis_t[...], chunks[slot], ((1,), (1,))))
        vcot = vcot_v[share(at, TILE), :]
        vproj[...] += dot_f32(high, vcot) + dot_f32(low, vcot)

        @pl.when(at < blocks - SLOTS)
        def _():
            chunk_copy(input_h, at + SLOTS, slot).start()

        @pl.when(at >= blocks - SLOTS)
        def _():
            chunk_copy(cot_h, at - (blocks - SLOTS), slot).start()

        @pl.when(at == SLOTS)
        def _():
            start_all(later)

        pl.when(at == 2)(enter)
        return carry

    lax.fori_loop(0, blocks, value_block, 0)
    start_all(vscatter)

    early[2].wait()
    obasis_t[...] = obasis_v[...].T

    def cot_block(at, carry):
        slot = lax.rem(at, SLOTS)
        chunk_copy(cot_h, at, slot).wait()
        high, low = split_two(dot_f32(obasis_t[...], chunks[slot], ((1,), (1,))))
        cb_high[at] = high
        cb_low[at] = low

        @pl.when(at < blocks - SLOTS)
        def _():
            chunk_copy(cot_h, at + SLOTS, slot).start()

        return carry

    lax.fori_loop(0, blocks, cot_block, 0)
    ring_forward(2, 0)
    for copy in attention:
        copy.wait()
    for head in range(pairs * PAIR):
        value_t[head] = value_v[:, head * DV : (head + 1) * DV].T

    last = PAIR * blocks
    lane = lax.broadcasted_iota(jnp.int32, (TILE, DV), 1)

    def head_columns(pair, which):
        return pl.ds(pl.multiple_of((pair * PAIR + which) * DV, DV), DV)

    def score_steps(item, pair):
        block, which = divmod(item, PAIR)
        slot = item % HELD
        columns = head_columns(pair, which)
        query = query_v[block * TILE : (block + 1) * TILE, columns].astype(F32)
        query = query * (DH ** (-0.5) * LOG2E)
        queries = [
            jnp.concatenate(split_two(part), axis=1)
            for part in (jnp.where(lane < DH, query, 0.0), jnp.where(lane < DH, 0.0, query))
        ]
        peaks = [jnp.full((8, TILE), -jnp.inf, F32)] * 2
        for tile in range(block + 1):
            span = slice(tile * TILE, (tile + 1) * TILE)
            keys = key_v[span, columns]
            keys = jnp.concatenate([keys, keys], axis=1)
            for which_map in range(2):
                one = dot_f32(keys, queries[which_map], ((1,), (1,)))
                if tile == block:
                    one = one + tri[...]
                scores[slot, which_map, span, :] = one
                peaks[which_map] = jnp.maximum(peaks[which_map], fold_rows(one, jnp.max))
            if tile == block:
                for which_map in range(2):
                    peak_ref[slot, which_map] = peaks[which_map]
            yield

    def exp_steps(item):
        slot = item % HELD
        peaks = [
            jnp.max(peak_ref[slot, which_map], axis=0, keepdims=True) for which_map in range(2)
        ]
        sums = [jnp.zeros((8, TILE), F32)] * 2
        last_tile = item // PAIR
        for tile in range(last_tile + 1):
            span = slice(tile * TILE, (tile + 1) * TILE)
            for which_map in range(2):
                one = jnp.exp2(scores[slot, which_map, span, :] - peaks[which_map])
                scores[slot, which_map, span, :] = one
                sums[which_map] += fold_rows(one, jnp.sum)
            if tile == last_tile:
                for which_map in range(2):
                    sum_ref[slot, which_map] = sums[which_map]
            yield

    def mix_steps(item, pair):
        block, which = divmod(item, PAIR)
        slot = item % HELD
        head = pair * PAIR + which
        width = (block + 1) * TILE
        rate_one = 1.0 / jnp.sum(sum_ref[slot, 0], axis=0, keepdims=True)
        rate_two = lam_ref[head] / jnp.sum(sum_ref[slot, 1], axis=0, keepdims=True)
        for tile in range(block + 1):
            span = slice(tile * TILE, (tile + 1) * TILE)
            mix_ref[span, :] = (
                scores[slot, 0, span, :] * rate_one - scores[slot, 1, span, :] * rate_two
            ).astype(BF16)
            if tile < block:
                yield
        raw = dot_f32(value_t[head, :, :width], mix_ref[:width, :])
        mean_sq = jnp.mean(raw * raw, axis=0, keepdims=True)
        gain = jnp.concatenate([gain_t[...]] * (TILE // DV), axis=1)
        out_t = (raw * lax.rsqrt(mean_sq + EPSILON_NORM) * gain).astype(BF16)
        span = slice(which * DV, (which + 1) * DV)
        oproj[pair, :, span] += dot_f32(cb_high[block], out_t, ((1,), (1,))) + dot_f32(
            cb_low[block], out_t, ((1,), (1,))
        )
        yield

    def together(*steps):
        live = list(steps)
        while live:
            live = [step for step in live if next(step, "done") != "done"]

    def attend(item, pair):
        before, ahead = (item - 1) % last, (item - 2) % last
        if item >= 2:
            together(
                mix_steps(ahead, pair), exp_steps(before), score_steps(item, pair)
            )
            return
        if item == 1:
            pl.when(pair > 0)(lambda: together(mix_steps(ahead, pair - 1)))
            together(exp_steps(before), score_steps(item, pair))
            return
        pl.when(pair > 0)(
            lambda: together(mix_steps(ahead, pair - 1), exp_steps(before))
        )
        together(score_steps(item, pair))

    events = {}

    def plan(pair, item, action):
        events.setdefault((pair, item), []).append(action)

    at = (13, 16, 18, 22, 25, 27)
    actions = (
        [value_moments]
        + [functools.partial(ring_forward, 3, step) for step in range(3)]
        + [value_squares, value_update]
    )

    def early_done():
        for step in range(3, half_count):
            ring_forward(2, step)
        out_copy(4 + 2 * pairs).start()

    plan(0, 12, functools.partial(ring_forward, 2, 1))
    plan(0, 15, functools.partial(ring_forward, 2, 2))
    plan(1, 4, early_done)
    for tick, action in zip(at, actions):
        plan(tick // last, tick % last, action)
    for pair in range(pairs - 1):
        plan(pair + 1, 10, functools.partial(start_all, oscatter[pair]))
        plan(pair + 1, 15, functools.partial(out_moments, pair))

    def pair_items(pair, carry):
        for item in range(last):
            for when in range(pairs):
                for action in events.get((when, item), []):
                    pl.when(pair == when)(action)
            attend(item, pair)
        return carry

    lax.fori_loop(0, pairs, pair_items, 0)
    together(mix_steps(last - 2, pairs - 1), exp_steps(last - 1))
    together(mix_steps(last - 1, pairs - 1))
    start_all(oscatter[pairs - 1])
    for (pair, item) in sorted(events):
        if pair >= pairs:
            for action in events[(pair, item)]:
                action()
    ring_forward(0, 0)
    for pair in range(pairs - 1):
        ring_forward(4 + pair, 0)
    out_moments(pairs - 1)
    ring_forward(0, 1)
    for step in range(half_count):
        ring_forward(3 + pairs, step)
        for pair in range(pairs - 1):
            if step + 1 < half_count:
                ring_forward(4 + pair, step + 1)
        if step + 2 < half_count:
            ring_forward(0, step + 2)
    for pair in range(pairs - 1):
        out_arrived(pair)
        out_step(pair)
    out_copy(3 + 2 * pairs).start()
    out_arrived(pairs - 1)
    out_update()
    for step in range(half_count):
        ring_forward(1, step)
        back = step + 1
        if step < half_count - 1:
            block_copy(owner(place - back)).start()
        block_copy(owner(place + back)).start()
    for copy in vscatter + square_copies(0) + square_copies(1):
        copy.wait_send()
    for at in range(pairs):
        for copy in oscatter[at]:
            copy.wait_send()
    for mat in range(4 + pairs):
        for step in range(half_count):
            for way in range(2):
                ring_copy(mat, step, way, False).wait_send()
    for index in range(len(sends)):
        out_copy(index).wait()
    for at in range(fs_count):
        block_copy(at).wait()


def finish_kernel(*refs):
    inputs, outputs, scratch = refs[:16], refs[16:26], refs[26:]
    in_sem, out_sem = scratch[-2:]
    held, results, early_copy = scratch[:16], scratch[16:24], scratch[24]
    (
        clips, vproj, oproj, ofirst, osecond, vfirst, vsecond, vdirs, odirs, obasis, vbasis,
        oweight, vweight, early_w, vcopy, ocopy,
    ) = held
    (
        ostep_o, vstep_o, onew_o, vnew_o, ocopy_o, vcopy_o, ofirst_o, osecond_o, vfirst_o,
        vsecond_o,
    ) = outputs
    ostep, vstep, onew, vnew, ofirst_new, osecond_new, vfirst_new, vsecond_new = results
    me = lax.axis_index("fs")
    row_share = vweight.shape[0]
    rows = pl.ds(pl.multiple_of(me * row_share, row_share), row_share)
    early_rows = early_w.shape[0]
    arrivals = [
        pltpu.make_async_copy(source, target, in_sem.at[index])
        for index, (source, target) in enumerate(zip(inputs, held))
    ]
    for copy in arrivals:
        copy.start()
    leaving = []

    def leave(source, target):
        copy = pltpu.make_async_copy(source, target, out_sem.at[len(leaving)])
        copy.start()
        leaving.append(copy)

    for index in range(14):
        arrivals[index].wait()
    clip_value = clips[0, :1, :1]
    clip_out = clips[1, :1, :1]
    pairs, rank, wide = odirs.shape
    out_parts = [split_two(odirs[at]) for at in range(pairs)]
    for start in range(0, early_rows, wide):
        count = min(wide, early_rows - start)
        high, low = out_parts[start // wide]
        high, low = high[:, :count], low[:, :count]
        step = dot_f32(high, obasis[...], ((0,), (1,))) + dot_f32(low, obasis[...], ((0,), (1,)))
        span = slice(start, start + count)
        early_copy[span, :] = (early_w[span, :] - LEARN_RATE * (clip_out * step)).astype(BF16)
    leave(early_copy, ocopy_o.at[pl.ds(0, early_rows)])
    arrivals[14].wait()
    leave(vcopy, vcopy_o)
    arrivals[15].wait()
    leave(ocopy, ocopy_o.at[pl.ds(early_rows, ocopy.shape[0])])
    high, low = split_two(vdirs[...])
    step = clip_value * (dot_f32(vbasis[rows, :], high) + dot_f32(vbasis[rows, :], low))
    vstep[...] = step
    leave(vstep, vstep_o)
    vnew[...] = vweight[...] - LEARN_RATE * step
    leave(vnew, vnew_o)
    for at in range(pairs):
        high, low = out_parts[at]
        step = clip_out * (
            dot_f32(high, obasis[rows, :], ((0,), (1,)))
            + dot_f32(low, obasis[rows, :], ((0,), (1,)))
        )
        span = slice(at * wide, (at + 1) * wide)
        ostep[span, :] = step
        onew[span, :] = oweight[span, :] - LEARN_RATE * step
        moments = moment_step(oproj[at], ofirst[:, span], osecond[:, span])
        ofirst_new[:, span] = moments[0]
        osecond_new[:, span] = moments[1]
    moments = moment_step(vproj[...], vfirst[...], vsecond[...])
    vfirst_new[...] = moments[0]
    vsecond_new[...] = moments[1]
    leave(ostep, ostep_o)
    leave(onew, onew_o)
    leave(ofirst_new, ofirst_o)
    leave(osecond_new, osecond_o)
    leave(vfirst_new, vfirst_o)
    leave(vsecond_new, vsecond_o)
    for copy in leaving:
        copy.wait()


def body(
    query_rows, key_rows, value_rows, mix_lambda, head_gain, out_cotangent, layer_input,
    value_cotangent, out_weight, value_weight, out_basis, value_basis, out_first, out_second,
    value_first, value_second,
):
    fs_count = lax.axis_size("fs")
    tp_count = lax.axis_size("tp")
    seq_len, cols = query_rows.shape
    width, rank = out_basis.shape
    row_share = value_weight.shape[0]
    rank_share = rank // fs_count
    heads = mix_lambda.shape[0]
    pairs = heads // PAIR
    blocks = seq_len // TILE
    half_count = fs_count // 2
    dma = pltpu.SemaphoreType.DMA
    like = lambda a: jax.ShapeDtypeStruct(a.shape, a.dtype)
    vmem = lambda a: pltpu.VMEM(a.shape, a.dtype)
    anywhere = pl.BlockSpec(memory_space=pl.ANY)
    early_rows = cols // EARLY
    early_shape = (early_rows, width)
    rest_shape = (cols - early_rows, width)
    vproj, oproj, vdirs, odirs, clips, vcopy, ocopy, early_w = pl.pallas_call(
        functools.partial(step_kernel, fs_count, tp_count),
        out_shape=(
            like(value_first),
            jax.ShapeDtypeStruct((pairs, rank_share, PAIR * DV), F32),
            jax.ShapeDtypeStruct((rank, cols), F32),
            jax.ShapeDtypeStruct((pairs, rank, PAIR * DV), F32),
            jax.ShapeDtypeStruct((2, 8, 128), F32),
            jax.ShapeDtypeStruct((width, cols), BF16),
            jax.ShapeDtypeStruct(rest_shape, BF16),
            jax.ShapeDtypeStruct(early_shape, F32),
        ),
        in_specs=[
            pl.BlockSpec(memory_space=pltpu.SMEM), pl.BlockSpec(memory_space=pltpu.VMEM),
        ] + [anywhere] * 14,
        out_specs=tuple([anywhere] * 8),
        scratch_shapes=[
            vmem(query_rows), vmem(key_rows), vmem(value_rows), vmem(value_cotangent),
            vmem(out_basis), vmem(value_basis), vmem(out_weight), vmem(value_weight),
            vmem(out_first), vmem(out_second), vmem(value_first), vmem(value_second),
            pltpu.VMEM((SLOTS, TILE, width), BF16),
            vmem(value_weight), vmem(out_weight), pltpu.VMEM((width, cols), BF16),
            pltpu.VMEM(rest_shape, BF16), pltpu.VMEM(early_shape, F32),
            pltpu.VMEM((2, 8, 128), F32),
            pltpu.VMEM((HELD, 2, seq_len, TILE), F32),
            pltpu.VMEM((HELD, 2, 8, TILE), F32),
            pltpu.VMEM((HELD, 2, 8, TILE), F32),
            pltpu.VMEM((seq_len, TILE), BF16),
            pltpu.VMEM((heads, DV, seq_len), BF16),
            pltpu.VMEM((rank, width), BF16),
            pltpu.VMEM((rank, width), BF16),
            pltpu.VMEM((blocks, rank, TILE), BF16),
            pltpu.VMEM((blocks, rank, TILE), BF16),
            pltpu.VMEM((DV, DV), F32),
            pltpu.VMEM((TILE, TILE), F32),
            pltpu.VMEM((rank, cols), F32),
            pltpu.VMEM((pairs, rank, PAIR * DV), F32),
            pltpu.VMEM((fs_count - 1, rank_share, cols), F32),
            pltpu.VMEM((pairs, fs_count - 1, rank_share, PAIR * DV), F32),
            pltpu.VMEM((rank, cols), F32),
            pltpu.VMEM((pairs, rank, PAIR * DV), F32),
            pltpu.VMEM((2, 8, 128), F32),
            pltpu.VMEM((2, tp_count - 1, 8, 128), F32),
            dma((13,)), dma((SLOTS,)),
            dma((fs_count - 1,)), dma((fs_count - 1,)),
            dma((pairs, fs_count - 1)), dma((pairs, fs_count - 1)),
            dma((2, tp_count - 1)), dma((2, tp_count - 1)),
            dma((4 + pairs, 2, half_count)), dma((4 + pairs, 2, half_count)),
            dma((5 + 2 * pairs,)), dma((fs_count,)),
        ],
        compiler_params=pltpu.CompilerParams(
            collective_id=0, has_side_effects=True, vmem_limit_bytes=62 * 1024 * 1024
        ),
        name="step",
    )(
        mix_lambda, head_gain.reshape(1, DV), query_rows, key_rows, value_rows, out_cotangent,
        layer_input, value_cotangent, out_basis, value_basis, out_weight, value_weight,
        out_first, out_second, value_first, value_second,
    )
    results = (
        like(out_weight), like(value_weight), like(out_weight), like(value_weight),
        jax.ShapeDtypeStruct((cols, width), BF16),
        jax.ShapeDtypeStruct((width, cols), BF16),
        like(out_first), like(out_second), like(value_first), like(value_second),
    )
    operands = (
        clips, vproj, oproj, out_first, out_second, value_first, value_second, vdirs, odirs,
        out_basis, value_basis, out_weight, value_weight, early_w, vcopy, ocopy,
    )
    return pl.pallas_call(
        finish_kernel,
        out_shape=results,
        in_specs=[anywhere] * len(operands),
        out_specs=tuple([anywhere] * len(results)),
        scratch_shapes=[vmem(a) for a in operands + results[:4] + results[6:]] + [
            pltpu.VMEM(early_shape, BF16), dma((len(operands),)), dma((11,)),
        ],
        compiler_params=pltpu.CompilerParams(vmem_limit_bytes=62 * 1024 * 1024),
        name="finish",
    )(*operands)


def solution(mesh):
    placed = (
        P("fs", "tp"),
        P("fs", "tp"),
        P("fs", "tp"),
        P("tp"),
        P(),
        P("fs", None),
        P("fs", None),
        P("fs", "tp"),
        P("tp", "fs"),
        P("fs", "tp"),
        P(),
        P(),
        P("fs", "tp"),
        P("fs", "tp"),
        P("fs", "tp"),
        P("fs", "tp"),
    )
    return jax.shard_map(
        body,
        mesh=mesh,
        in_specs=placed,
        out_specs=(
            P("tp", "fs"),
            P("fs", "tp"),
            P("tp", "fs"),
            P("fs", "tp"),
            P("tp", None),
            P(None, "tp"),
            P("fs", "tp"),
            P("fs", "tp"),
            P("fs", "tp"),
            P("fs", "tp"),
        ),
        check_vma=False,
    )
```
